32 devices in a mesh: gr: 2 (over core), fs: 8 (over z, y), tp: 2 (over x).
Axes of the slice: x: 2, y: 2, z: 4, core: 2. Of those that a mesh axis runs over, the one named last changes fastest.
Arguments:
- tokens: bfloat16 [2048, 2048], P(('gr', 'fs')), may hold values from -60 to 60
- route_ids: int32 [2048, 2], P(('gr', 'fs')), may hold values from 0 to 7, all different within a row; in each aligned block of 128 rows (0 to 127, 128 to 255, ...) at most 32 rows name the same one
- route_logits: float32 [2048, 2], P(('gr', 'fs')), may hold values from -8 to 8
- norm_gain: float32 [2048], P(('gr', 'fs')), may hold values from 0.1 to 1.9
- gate_master: float32 [8, 2048, 7168], P(None, ('gr', 'fs'), 'tp'), may hold values from -0.125 to 0.125
- up_master: float32 [8, 2048, 7168], P(None, ('gr', 'fs'), 'tp'), may hold values from -0.125 to 0.125
- down_master: float32 [8, 7168, 2048], P(None, 'fs', ('gr', 'tp')), may hold values from -0.0625 to 0.0625
Outputs:
- gate_weight: bfloat16 [8, 2048, 7168], P('tp', None, 'fs')
- up_weight: bfloat16 [8, 2048, 7168], P('tp', None, 'fs')
- down_weight: bfloat16 [8, 7168, 2048], P('tp', 'fs')
- mixed: bfloat16 [2048, 2048], P(('gr', 'fs'))
The draws below stay inside these ranges and needn't reach their ends.
Inputs may be any that keep to these rules, and one draw needn't show every extreme that they name: `route_ids`: in the rows of one device, that is in each aligned block of 128 rows, each of the 8 experts is named by exactly 32 rows; a row names two different experts.
All inputs are finite; a program needn't handle non-finite values.
Results may differ from the reference program's by a relative error of at most 0.025.
Values may be sent and summed in bfloat16 or wider, within the bound.
A program may use at most 192 MiB of HBM per device.

```python
import math
import jax
import jax.numpy as jnp
import numpy as np
from jax import lax

D = 2048
FF = 7168
EXPERTS = 8
TOK_DEV = 128
CAP = 32
TOKENS = 2048
N_FS = 8
N_TP = 2


def draw_tokens(key, part):
    first_key = jax.random.fold_in(key, 11)
    second_key = jax.random.fold_in(key, 12)
    values = jnp.clip(jax.random.normal(first_key, (TOKENS, D), jnp.float32), -4.0, 4.0)
    scales = jnp.exp(jax.random.uniform(second_key, (TOKENS, 1), jnp.float32, 0.0, math.log(10.0)))
    return (values * scales).astype(jnp.bfloat16)


def level_of(own_key, shape, pieces, smallest, largest):
    loudness, own = 1.0, jax.random.fold_in(own_key, 6)
    for position, parts in pieces:
        heights = jnp.exp(jax.random.uniform(jax.random.fold_in(own, position), (parts,), jnp.float32, smallest / len(pieces), largest / len(pieces)))
        loudness = loudness * jnp.repeat(heights, shape[position] // parts).reshape([-1 if axis == position else 1 for axis in range(len(shape))])
    return loudness


def shared_out(rng, own, number, rows, count, top, reach, lean):
    order = jax.random.permutation(rng, count)
    crowded, usual = portions_of(count, rows * top, reach, lean, True), portions_of(count, rows * top, reach, lean, False)
    places = jnp.arange(count)

    def named(tallies, rotation):
        used = int((tallies > 0).sum())
        fixed = max(1, used // 4)
        passed = fixed + (places - fixed + rotation * (used - fixed)) % max(1, count - fixed)
        return jnp.zeros((count,), jnp.int32).at[order[jnp.where(places < fixed, places, passed)]].set(jnp.asarray(tallies, jnp.int32))

    tallies = jnp.where(number % 4 == 0, named(crowded, number // 4), named(usual, number - number // 4 - 1))
    mixed = jax.random.permutation(jax.random.fold_in(own, 3), count)
    giver, sink = mixed[0:count // 2 * 2:2], mixed[1:count // 2 * 2:2]
    margin = jnp.minimum(tallies[giver] - 1, reach - tallies[sink]) // 2
    margin = jnp.where((giver == order[0]) | (sink == order[0]) | (tallies[sink] == 0), 0, jnp.maximum(margin, 0))
    passed = jax.random.randint(jax.random.fold_in(own, 4), (count // 2,), 0, 1 << 20) % (margin + 1)
    tallies = tallies.at[giver].add(-passed).at[sink].add(passed)
    labels = jnp.searchsorted(jnp.cumsum(tallies), jnp.arange(rows * top), side="right").astype(jnp.int32)
    table = labels.reshape(top, rows).T
    table = table[jax.random.permutation(jax.random.fold_in(own, 1), rows)]
    rotation = jax.random.randint(jax.random.fold_in(own, 2), (rows, 1), 0, top)
    return jnp.take_along_axis(table, (jnp.arange(top)[None, :] + rotation) % top, axis=1)


def portions_of(number_of, total, reach, slope, full):
    portions = [(1 << 20) // math.isqrt(rank ** slope) + 1 for rank in range(1, number_of + 1)]
    largest = reach if full else min(reach, max(-(-total // number_of), total * portions[0] // sum(portions)))
    least = 1 if total - largest >= number_of - 1 else 0
    holding, rest = [largest] + [least] * (number_of - 1), total - largest - least * (number_of - 1)
    while rest > 0:
        movable = [i for i in range(1, number_of) if holding[i] < largest] or [i for i in range(1, number_of) if holding[i] < reach]
        whole, budget = sum([portions[i] for i in movable]), rest
        for i in movable:
            extra = min(reach - holding[i], max(1, budget * portions[i] // whole), rest)
            holding[i] = holding[i] + extra
            rest = rest - extra
    return np.array(holding)


def scatter_about(stream_key, dims, scale, limit, cuts=(), kind=jnp.bfloat16):
    loudness = level_of(stream_key, dims, cuts, -0.22, 0.18) if cuts else 1.0
    array = jax.random.normal(stream_key, dims, jnp.float32) * scale * loudness
    return jnp.minimum(jnp.maximum(array, -limit), limit).astype(kind)


def setup_inputs(seed: int = 0) -> dict:
    keys = jax.random.split(jax.random.key(seed), 8)
    tokens = draw_tokens(jax.random.fold_in(keys[7], 71), 0)
    route_ids_keys = jax.random.split(jax.random.fold_in(keys[1], 1), TOKENS // TOK_DEV)
    route_ids_turns = jax.random.permutation(jax.random.fold_in(keys[1], 3), TOKENS // TOK_DEV)
    route_ids = jax.vmap(lambda own, number: shared_out(jax.random.fold_in(keys[1], 2), own, number, TOK_DEV, EXPERTS, 2, CAP, 1))(route_ids_keys, route_ids_turns).reshape((TOKENS, 2))
    route_logits = scatter_about(keys[2], (TOKENS, 2), 1.5, 8.0, ((0, 16),), jnp.float32)
    norm_gain = jnp.clip(1.0 + 0.18 * jax.random.normal(keys[3], (D,), jnp.float32), 0.1, 1.9)
    gate_master = scatter_about(keys[4], (EXPERTS, D, FF), D ** -0.5, 0.125, ((1, 16), (2, 2)), jnp.float32)
    up_master = scatter_about(keys[5], (EXPERTS, D, FF), D ** -0.5, 0.125, ((1, 16), (2, 2)), jnp.float32)
    down_master = scatter_about(keys[6], (EXPERTS, FF, D), FF ** -0.5, 0.0625, ((1, 8), (2, 4)), jnp.float32)
    return {"tokens": tokens, "route_ids": route_ids, "route_logits": route_logits, "norm_gain": norm_gain, "gate_master": gate_master, "up_master": up_master, "down_master": down_master}


epsilon = 1e-06

def reference(tokens, route_ids, route_logits, norm_gain, gate_master, up_master, down_master):
    gate_weight = (gate_master * norm_gain[None, :, None]).astype(jnp.bfloat16)
    up_weight = (up_master * norm_gain[None, :, None]).astype(jnp.bfloat16)
    down_weight = down_master.astype(jnp.bfloat16)
    as_float = tokens.astype(jnp.float32)
    normed = (as_float * lax.rsqrt(lax.optimization_barrier(jnp.mean(as_float * as_float, axis=-1, keepdims=True)) + epsilon)).astype(jnp.bfloat16)
    differ = route_logits[:, 0] - route_logits[:, 1]
    route_weight = jnp.stack([jax.nn.sigmoid(differ), jax.nn.sigmoid(-differ)], axis=1)
    routed = TOKENS // 4
    positions = jnp.arange(TOKENS, dtype=jnp.int32)
    slice_width = FF // N_FS
    per_block = EXPERTS // N_TP

    def expert_part(expert):
        route_hits = route_ids == expert
        chosen = jnp.any(route_hits, axis=1)
        sort_key = jnp.where(chosen, positions, positions + TOKENS)
        order = jnp.argsort(sort_key)[:routed].astype(jnp.int32)
        weight_rows = lax.optimization_barrier(jnp.sum(jnp.where(route_hits, route_weight, 0.0), axis=1))[order]
        picked = normed[order]
        gate_act = jnp.dot(picked, gate_weight[expert], preferred_element_type=jnp.float32)
        up_act = jnp.dot(picked, up_weight[expert], preferred_element_type=jnp.float32)
        hidden = (jax.nn.silu(gate_act) * up_act).astype(jnp.bfloat16)
        down_expert = down_weight[expert]

        def add_slice(summed, slice_idx):
            begin = (slice_idx * slice_width).astype(jnp.int32)
            hidden_slice = lax.dynamic_slice_in_dim(hidden, begin, slice_width, 1)
            down_slice = lax.dynamic_slice_in_dim(down_expert, begin, slice_width, 0)
            partial_value = jnp.dot(hidden_slice, down_slice, preferred_element_type=jnp.float32)
            rounded = lax.optimization_barrier(partial_value.astype(jnp.bfloat16)).astype(jnp.float32)
            return (summed + rounded, None)
        expert_out, _ = lax.scan(add_slice, jnp.zeros((routed, D), jnp.float32), jnp.arange(N_FS, dtype=jnp.int32))
        return jnp.zeros((TOKENS, D), jnp.float32).at[order].add(expert_out * weight_rows[:, None])
    summed_all = jnp.zeros((TOKENS, D), jnp.float32)
    for tp_block in range(N_TP):
        block_sum = jnp.zeros((TOKENS, D), jnp.float32)
        for member in range(per_block):
            block_sum = block_sum + expert_part(tp_block * per_block + member)
        summed_all = summed_all + lax.optimization_barrier(block_sum.astype(jnp.bfloat16)).astype(jnp.float32)
    mixed = summed_all.astype(jnp.bfloat16)
    return (gate_weight, up_weight, down_weight, mixed)
```

```python
import functools

import jax
import jax.numpy as jnp
from jax import lax
from jax.experimental import pallas as pl
from jax.experimental.pallas import tpu as pltpu
from jax.sharding import PartitionSpec as P

CAP = 32


epsilon = 1e-06
MESH = pl.DeviceIdType.MESH
BF16 = jnp.bfloat16


def exchange_kernel(
    n_gr, n_fs, n_tp,
    gain_ref, gate_ref, up_ref, down_ref,
    gate_out, up_out, down_out,
    stage, stage_down, crossed, raw, raw_down,
    load_sem, load_down_sem, x_send, x_recv, s_send, s_recv, own_sem,
    d_send, d_recv, xd_send, xd_recv, own_down_sem, dd_send, dd_recv,
):
    gr, fs, tp = (lax.axis_index(name) for name in ("gr", "fs", "tp"))
    experts, _, width = gate_out.shape
    rows, cols = gate_ref.shape[1], gate_ref.shape[2]
    per = cols // width
    down_cols = down_ref.shape[2]
    masters, outs = (gate_ref, up_ref), (gate_out, up_out)

    barrier = pltpu.get_barrier_semaphore()
    peers = 0
    for o in range(1, n_tp):
        pl.semaphore_signal(barrier, 1, device_id=(gr, fs, lax.rem(tp + o, n_tp)), device_id_type=MESH)
        peers += 1
    for k in range(1, n_fs):
        pl.semaphore_signal(barrier, 1, device_id=(gr, lax.rem(fs + k, n_fs), tp), device_id_type=MESH)
        peers += 1
    for o in range(1, n_gr):
        pl.semaphore_signal(barrier, 1, device_id=(lax.rem(gr + o, n_gr), fs, tp), device_id_type=MESH)
        peers += 1

    def tp_at(o):
        return lax.rem(tp + o, n_tp)

    order = [(w, o) for w in range(2) for o in [*range(1, n_tp), 0]]

    def load(e, w, o):
        return pltpu.make_async_copy(
            masters[w].at[tp_at(o) * experts + e], raw.at[w, o], load_sem.at[w, o]
        )

    def load_down(e, o):
        return pltpu.make_async_copy(
            down_ref.at[tp_at(o) * experts + e], raw_down.at[o], load_down_sem.at[o]
        )

    def over_tp(e, w, o):
        return pltpu.make_async_remote_copy(
            stage.at[w, o, e], crossed.at[w, o - 1, e],
            x_send.at[w, o - 1, e], x_recv.at[w, o - 1, e],
            device_id=(gr, fs, tp_at(o)), device_id_type=MESH,
        )

    def rows_of(group, owner):
        return pl.ds(pl.multiple_of((group * n_fs + owner) * rows, rows), rows)

    def source(e, w, o, j):
        columns = pl.ds(j * width, width)
        if o == 0:
            return stage.at[w, 0, e, :, columns]
        return crossed.at[w, o - 1, e, :, columns]

    def fan(e, w, o):
        begin = lax.rem(tp - o + n_tp, n_tp) * per
        for j in range(per):
            to = begin + j
            k = lax.rem(to - fs + n_fs, n_fs)
            target = outs[w].at[e, rows_of(gr, fs)]

            @pl.when(to != fs)
            def _():
                pltpu.make_async_remote_copy(
                    source(e, w, o, j), target, s_send.at[w, e, k], s_recv.at[w, e, k],
                    device_id=(gr, to, tp), device_id_type=MESH,
                ).start()

            @pl.when(to == fs)
            def _():
                pltpu.make_async_copy(source(e, w, o, j), target, own_sem.at[w, e]).start()

    def arrival(e, w, k):
        piece = outs[w].at[e, rows_of(gr, lax.rem(fs - k + n_fs, n_fs))]
        return pltpu.make_async_remote_copy(
            piece, piece, s_send.at[w, e, k], s_recv.at[w, e, k],
            device_id=(gr, lax.rem(fs + k, n_fs), tp), device_id_type=MESH,
        )

    def own_copy(e, w):
        return pltpu.make_async_copy(
            source(e, w, 0, 0), outs[w].at[e, rows_of(gr, fs)], own_sem.at[w, e]
        )

    def over_gr(e, w, k, o, group):
        piece = outs[w].at[e, rows_of(group, lax.rem(fs - k + n_fs, n_fs))]
        return pltpu.make_async_remote_copy(
            piece, piece, d_send.at[w, e, k, o - 1], d_recv.at[w, e, k, o - 1],
            device_id=(lax.rem(gr + o, n_gr), fs, tp), device_id_type=MESH,
        )

    def down_block(group, t):
        return pl.ds(pl.multiple_of((group * n_tp + t) * down_cols, down_cols), down_cols)

    def down_over_tp(e, o):
        return pltpu.make_async_remote_copy(
            stage_down.at[o, e], down_out.at[e, :, down_block(gr, tp)],
            xd_send.at[o - 1, e], xd_recv.at[o - 1, e],
            device_id=(gr, fs, tp_at(o)), device_id_type=MESH,
        )

    def down_arrival(e, o):
        piece = down_out.at[e, :, down_block(gr, lax.rem(tp - o + n_tp, n_tp))]
        return pltpu.make_async_remote_copy(
            piece, piece, xd_send.at[o - 1, e], xd_recv.at[o - 1, e],
            device_id=(gr, fs, tp_at(o)), device_id_type=MESH,
        )

    def down_own(e):
        return pltpu.make_async_copy(
            stage_down.at[0, e], down_out.at[e, :, down_block(gr, tp)], own_down_sem.at[e]
        )

    def down_over_gr(e, s, o, group):
        piece = down_out.at[e, :, down_block(group, lax.rem(tp - s + n_tp, n_tp))]
        return pltpu.make_async_remote_copy(
            piece, piece, dd_send.at[e, s, o - 1], dd_recv.at[e, s, o - 1],
            device_id=(lax.rem(gr + o, n_gr), fs, tp), device_id_type=MESH,
        )

    for w, o in order:
        load(0, w, o).start()
    for o in range(n_tp):
        load_down(0, o).start()
    pl.semaphore_wait(barrier, peers)

    @pl.loop(0, experts)
    def _(e):
        for w, o in order:
            load(e, w, o).wait()
            stage[w, o, e] = (raw[w, o] * gain_ref[...]).astype(BF16)

            @pl.when(e + 1 < experts)
            def _():
                load(e + 1, w, o).start()

            if o:
                over_tp(e, w, o).start()
            else:
                fan(e, w, 0)

    @pl.loop(0, experts)
    def _(e):
        for o in [*range(1, n_tp), 0]:
            load_down(e, o).wait()
            stage_down[o, e] = raw_down[o].astype(BF16)

            @pl.when(e + 1 < experts)
            def _():
                load_down(e + 1, o).start()

            if o:
                down_over_tp(e, o).start()
            else:
                down_own(e).start()

    def forward(e):
        for w in range(2):
            for o in range(1, n_tp):
                over_tp(e, w, o).wait_recv()
                fan(e, w, o)

    def collect(e):
        for w in range(2):
            own_copy(e, w).wait()
            for o in range(1, n_gr):
                over_gr(e, w, 0, o, gr).start()

        @pl.loop(1, n_fs)
        def _(k):
            for w in range(2):
                arrival(e, w, k).wait_recv()
                for o in range(1, n_gr):
                    over_gr(e, w, k, o, gr).start()

    forward(0)

    @pl.loop(1, experts)
    def _(e):
        forward(e)
        collect(e - 1)

    @pl.loop(0, experts)
    def _(e):
        down_own(e).wait()
        for s in range(1, n_tp):
            down_arrival(e, s).wait_recv()
        for s in range(n_tp):
            for o in range(1, n_gr):
                down_over_gr(e, s, o, gr).start()

    collect(experts - 1)

    @pl.loop(0, experts)
    def _(e):
        for w in range(2):
            for o in range(1, n_tp):
                over_tp(e, w, o).wait_send()

            @pl.loop(1, n_fs)
            def _(k):
                arrival(e, w, k).wait_send()

            @pl.loop(0, n_fs)
            def _(k):
                for o in range(1, n_gr):
                    over_gr(e, w, k, o, gr).wait_send()
                    over_gr(e, w, k, o, lax.rem(gr - o + n_gr, n_gr)).wait_recv()

        for s in range(1, n_tp):
            down_over_tp(e, s).wait_send()
        for s in range(n_tp):
            for o in range(1, n_gr):
                down_over_gr(e, s, o, gr).wait_send()
                down_over_gr(e, s, o, lax.rem(gr - o + n_gr, n_gr)).wait_recv()


def exchange(sizes, norm_gain, gate_master, up_master, down_master):
    n_gr, n_fs, n_tp = sizes
    all_experts, rows, cols = gate_master.shape
    experts = all_experts // n_tp
    width = cols * n_tp // n_fs
    hidden, down_cols = down_master.shape[1], down_master.shape[2]
    any_spec = pl.BlockSpec(memory_space=pl.ANY)
    dma = pltpu.SemaphoreType.DMA
    up_shape = jax.ShapeDtypeStruct((experts, rows * n_gr * n_fs, width), BF16)
    return pl.pallas_call(
        functools.partial(exchange_kernel, n_gr, n_fs, n_tp),
        out_shape=(
            up_shape,
            up_shape,
            jax.ShapeDtypeStruct((experts, hidden, down_cols * n_gr * n_tp), BF16),
        ),
        in_specs=[pl.BlockSpec(memory_space=pltpu.VMEM), any_spec, any_spec, any_spec],
        out_specs=(any_spec, any_spec, any_spec),
        scratch_shapes=[
            pltpu.VMEM((2, n_tp, experts, rows, cols), BF16),
            pltpu.VMEM((n_tp, experts, hidden, down_cols), BF16),
            pltpu.VMEM((2, n_tp - 1, experts, rows, cols), BF16),
            pltpu.VMEM((2, n_tp, rows, cols), jnp.float32),
            pltpu.VMEM((n_tp, hidden, down_cols), jnp.float32),
            dma((2, n_tp)),
            dma((n_tp,)),
            dma((2, n_tp - 1, experts)),
            dma((2, n_tp - 1, experts)),
            dma((2, experts, n_fs)),
            dma((2, experts, n_fs)),
            dma((2, experts)),
            dma((2, experts, n_fs, n_gr - 1)),
            dma((2, experts, n_fs, n_gr - 1)),
            dma((n_tp - 1, experts)),
            dma((n_tp - 1, experts)),
            dma((experts,)),
            dma((experts, n_tp, n_gr - 1)),
            dma((experts, n_tp, n_gr - 1)),
        ],
        compiler_params=pltpu.CompilerParams(
            collective_id=0, has_side_effects=True, vmem_limit_bytes=52 * 1024 * 1024
        ),
        cost_estimate=pl.CostEstimate(flops=0, bytes_accessed=1_000_000_000, transcendentals=0),
    )(norm_gain[:, None], gate_master, up_master, down_master)


def plain_local(tokens, route_ids, route_logits, norm_gain, gate_master, up_master, down_master):
    gain_rows = norm_gain[None, :, None]
    gate_half = (gate_master * gain_rows).astype(jnp.bfloat16)
    up_half = (up_master * gain_rows).astype(jnp.bfloat16)
    down_half = down_master.astype(jnp.bfloat16)
    gate_cols, up_cols, down_cols = (
        lax.all_to_all(gate_half, "tp", split_axis=0, concat_axis=2, tiled=True),
        lax.all_to_all(up_half, "tp", split_axis=0, concat_axis=2, tiled=True),
        lax.all_to_all(down_half, "tp", split_axis=0, concat_axis=2, tiled=True),
    )
    gate_part, up_part = (
        lax.all_to_all(gate_cols, "fs", split_axis=2, concat_axis=1, tiled=True),
        lax.all_to_all(up_cols, "fs", split_axis=2, concat_axis=1, tiled=True),
    )
    gate_weight, up_weight, down_weight = (
        lax.all_gather(gate_part, "gr", axis=1, tiled=True),
        lax.all_gather(up_part, "gr", axis=1, tiled=True),
        lax.all_gather(down_cols, "gr", axis=2, tiled=True),
    )
    as_float = tokens.astype(jnp.float32)
    normed = (
        as_float * lax.rsqrt(jnp.mean(as_float * as_float, axis=-1, keepdims=True) + epsilon)
    ).astype(jnp.bfloat16)
    differ = route_logits[:, 0] - route_logits[:, 1]
    route_weight = jnp.stack([jax.nn.sigmoid(differ), jax.nn.sigmoid(-differ)], axis=1)
    experts_here = gate_weight.shape[0]
    first_expert = lax.axis_index("tp") * experts_here
    expert_ids = first_expert + jnp.arange(experts_here, dtype=jnp.int32)
    route_hits = route_ids[None, :, :] == expert_ids[:, None, None]
    chosen = jnp.any(route_hits, axis=2)
    weight_rows = jnp.sum(jnp.where(route_hits, route_weight[None, :, :], 0.0), axis=2)
    slot_rank = jnp.cumsum(chosen.astype(jnp.int32), axis=1) - 1
    slot_ids = jnp.arange(CAP, dtype=jnp.int32)
    picker = chosen[:, None, :] & (slot_rank[:, None, :] == slot_ids[None, :, None])
    picker_float = picker.astype(jnp.float32)
    packed = jnp.einsum(
        "xsr,rd->sxd", picker.astype(jnp.bfloat16), normed, preferred_element_type=jnp.float32
    ).astype(jnp.bfloat16)
    slot_weight = jnp.einsum(
        "xsr,xr->sx", picker_float, weight_rows, precision=lax.Precision.HIGHEST
    )
    pieces = lax.all_gather(packed, "fs", axis=0, tiled=True)
    gate_act = jnp.einsum("kxd,xdh->kxh", pieces, gate_weight, preferred_element_type=jnp.float32)
    up_act = jnp.einsum("kxd,xdh->kxh", pieces, up_weight, preferred_element_type=jnp.float32)
    hidden = (jax.nn.silu(gate_act) * up_act).astype(jnp.bfloat16)
    expert_out = lax.psum_scatter(
        jnp.einsum("kxh,xhd->kxd", hidden, down_weight, preferred_element_type=jnp.float32).astype(
            jnp.bfloat16
        ),
        "fs",
        scatter_dimension=0,
        tiled=True,
    ).astype(jnp.float32)
    weighted = expert_out * slot_weight[:, :, None]
    block_sum = jnp.einsum("xsr,sxd->rd", picker_float, weighted, precision=lax.Precision.HIGHEST)
    mixed = lax.psum(block_sum.astype(jnp.bfloat16), "tp")
    return (gate_weight, up_weight, down_weight, mixed)


def fast_local(sizes, tokens, route_ids, route_logits, norm_gain, gate_master, up_master, down_master):
    n_gr, n_fs, n_tp = sizes
    gate_weight, up_weight, down_weight = exchange(
        sizes, norm_gain, gate_master, up_master, down_master
    )
    as_float = tokens.astype(jnp.float32)
    normed = (
        as_float * lax.rsqrt(jnp.mean(as_float * as_float, axis=-1, keepdims=True) + epsilon)
    ).astype(jnp.bfloat16)
    differ = route_logits[:, 0] - route_logits[:, 1]
    route_weight = jnp.stack([jax.nn.sigmoid(differ), jax.nn.sigmoid(-differ)], axis=1)
    experts_here = gate_weight.shape[0]
    first_expert = lax.axis_index("tp") * experts_here
    expert_ids = first_expert + jnp.arange(experts_here, dtype=jnp.int32)
    route_hits = route_ids[None, :, :] == expert_ids[:, None, None]
    chosen = jnp.any(route_hits, axis=2)
    weight_rows = jnp.sum(jnp.where(route_hits, route_weight[None, :, :], 0.0), axis=2)
    slot_rank = jnp.cumsum(chosen.astype(jnp.int32), axis=1) - 1
    slot_ids = jnp.arange(CAP, dtype=jnp.int32)
    picker = chosen[:, None, :] & (slot_rank[:, None, :] == slot_ids[None, :, None])
    picker_float = picker.astype(jnp.float32)
    packed = jnp.einsum(
        "xsr,rd->sxd", picker.astype(jnp.bfloat16), normed, preferred_element_type=jnp.float32
    ).astype(jnp.bfloat16)
    slot_weight = jnp.einsum(
        "xsr,xr->sx", picker_float, weight_rows, precision=lax.Precision.HIGHEST
    )
    pieces = lax.all_gather(packed, "fs", axis=0, tiled=True)
    gate_act = jnp.einsum("kxd,xdh->kxh", pieces, gate_weight, preferred_element_type=jnp.float32)
    up_act = jnp.einsum("kxd,xdh->kxh", pieces, up_weight, preferred_element_type=jnp.float32)
    hidden = (jax.nn.silu(gate_act) * up_act).astype(jnp.bfloat16)
    partial = jnp.einsum(
        "kxh,xhd->kxd", hidden, down_weight, preferred_element_type=jnp.float32
    ).astype(jnp.bfloat16)
    pairs, rest = n_fs // 2, (partial.shape[0] // n_fs, *partial.shape[1:])
    partial = lax.psum_scatter(
        partial.reshape(pairs, 2, *rest), "fs", scatter_dimension=1,
        axis_index_groups=[[2 * i, 2 * i + 1] for i in range(pairs)],
    )
    expert_out = lax.psum_scatter(
        partial, "fs", scatter_dimension=0,
        axis_index_groups=[[2 * i + j for i in range(pairs)] for j in range(2)],
    ).astype(jnp.float32)
    weighted = expert_out * slot_weight[:, :, None]
    block_sum = jnp.einsum("xsr,sxd->rd", picker_float, weighted, precision=lax.Precision.HIGHEST)
    mixed = lax.psum(block_sum.astype(jnp.bfloat16), "tp")
    return (gate_weight, up_weight, down_weight, mixed)


def solution(mesh):
    n_gr, n_fs, n_tp = (mesh.shape[name] for name in ("gr", "fs", "tp"))
    placed = (
        P(("gr", "fs"), None),
        P(("gr", "fs"), None),
        P(("gr", "fs"), None),
        P(("gr", "fs")),
        P(None, ("gr", "fs"), "tp"),
        P(None, ("gr", "fs"), "tp"),
        P(None, "fs", ("gr", "tp")),
    )

    def local(tokens, route_ids, route_logits, norm_gain, gate_master, up_master, down_master):
        width = gate_master.shape[2] * n_tp // n_fs
        aligned = width % 128 == 0 and down_master.shape[2] % 128 == 0
        fits = n_fs % n_tp == 0 and n_fs % 2 == 0 and min(n_gr, n_tp) > 1
        run = functools.partial(fast_local, (n_gr, n_fs, n_tp)) if aligned and fits else plain_local
        return run(tokens, route_ids, route_logits, norm_gain, gate_master, up_master, down_master)

    return jax.shard_map(
        local,
        mesh=mesh,
        in_specs=placed,
        out_specs=(
            P("tp", None, "fs"),
            P("tp", None, "fs"),
            P("tp", "fs", None),
            P(("gr", "fs"), None),
        ),
        check_vma=False,
    )
```

```python
import functools

import jax
import jax.numpy as jnp
from jax import lax
from jax.experimental import pallas as pl
from jax.experimental.pallas import tpu as pltpu
from jax.sharding import PartitionSpec as P

CAP = 32


epsilon = 1e-06
MESH = pl.DeviceIdType.MESH
BF16 = jnp.bfloat16


def exchange_kernel(
    n_gr, n_fs, n_tp,
    gain_ref, gate_ref, up_ref, down_ref,
    gate_out, up_out, down_out,
    stage, stage_down, crossed, raw, raw_down,
    load_sem, load_down_sem, x_send, x_recv, s_send, s_recv, own_sem,
    d_send, d_recv, xd_send, xd_recv, own_down_sem, dd_send, dd_recv,
):
    gr, fs, tp = (lax.axis_index(name) for name in ("gr", "fs", "tp"))
    experts, _, width = gate_out.shape
    rows, cols = gate_ref.shape[1], gate_ref.shape[2]
    per = cols // width
    down_cols = down_ref.shape[2]
    masters, outs = (gate_ref, up_ref), (gate_out, up_out)

    barrier = pltpu.get_barrier_semaphore()
    peers = 0
    for o in range(1, n_tp):
        pl.semaphore_signal(barrier, 1, device_id=(gr, fs, lax.rem(tp + o, n_tp)), device_id_type=MESH)
        peers += 1
    for k in range(1, n_fs):
        pl.semaphore_signal(barrier, 1, device_id=(gr, lax.rem(fs + k, n_fs), tp), device_id_type=MESH)
        peers += 1
    for o in range(1, n_gr):
        pl.semaphore_signal(barrier, 1, device_id=(lax.rem(gr + o, n_gr), fs, tp), device_id_type=MESH)
        peers += 1

    def tp_at(o):
        return lax.rem(tp + o, n_tp)

    order = [(w, o) for w in range(2) for o in [*range(1, n_tp), 0]]

    def load(e, w, o):
        return pltpu.make_async_copy(
            masters[w].at[tp_at(o) * experts + e], raw.at[w, o], load_sem.at[w, o]
        )

    def load_down(e, o):
        return pltpu.make_async_copy(
            down_ref.at[tp_at(o) * experts + e], raw_down.at[o], load_down_sem.at[o]
        )

    def over_tp(e, w, o):
        return pltpu.make_async_remote_copy(
            stage.at[w, o, e], crossed.at[w, o - 1, e],
            x_send.at[w, o - 1, e], x_recv.at[w, o - 1, e],
            device_id=(gr, fs, tp_at(o)), device_id_type=MESH,
        )

    def rows_of(group, owner):
        return pl.ds(pl.multiple_of((group * n_fs + owner) * rows, rows), rows)

    def source(e, w, o, j):
        columns = pl.ds(j * width, width)
        if o == 0:
            return stage.at[w, 0, e, :, columns]
        return crossed.at[w, o - 1, e, :, columns]

    def fan(e, w, o):
        begin = lax.rem(tp - o + n_tp, n_tp) * per
        for j in range(per):
            to = begin + j
            k = lax.rem(to - fs + n_fs, n_fs)
            target = outs[w].at[e, rows_of(gr, fs)]

            @pl.when(to != fs)
            def _():
                pltpu.make_async_remote_copy(
                    source(e, w, o, j), target, s_send.at[w, e, k], s_recv.at[w, e, k],
                    device_id=(gr, to, tp), device_id_type=MESH,
                ).start()

            @pl.when(to == fs)
            def _():
                pltpu.make_async_copy(source(e, w, o, j), target, own_sem.at[w, e]).start()

    def arrival(e, w, k):
        piece = outs[w].at[e, rows_of(gr, lax.rem(fs - k + n_fs, n_fs))]
        return pltpu.make_async_remote_copy(
            piece, piece, s_send.at[w, e, k], s_recv.at[w, e, k],
            device_id=(gr, lax.rem(fs + k, n_fs), tp), device_id_type=MESH,
        )

    def own_copy(e, w):
        return pltpu.make_async_copy(
            source(e, w, 0, 0), outs[w].at[e, rows_of(gr, fs)], own_sem.at[w, e]
        )

    def over_gr(e, w, k, o, group):
        piece = outs[w].at[e, rows_of(group, lax.rem(fs - k + n_fs, n_fs))]
        return pltpu.make_async_remote_copy(
            piece, piece, d_send.at[w, e, k, o - 1], d_recv.at[w, e, k, o - 1],
            device_id=(lax.rem(gr + o, n_gr), fs, tp), device_id_type=MESH,
        )

    def down_block(group, t):
        return pl.ds(pl.multiple_of((group * n_tp + t) * down_cols, down_cols), down_cols)

    def down_over_tp(e, o):
        return pltpu.make_async_remote_copy(
            stage_down.at[o, e], down_out.at[e, :, down_block(gr, tp)],
            xd_send.at[o - 1, e], xd_recv.at[o - 1, e],
            device_id=(gr, fs, tp_at(o)), device_id_type=MESH,
        )

    def down_arrival(e, o):
        piece = down_out.at[e, :, down_block(gr, lax.rem(tp - o + n_tp, n_tp))]
        return pltpu.make_async_remote_copy(
            piece, piece, xd_send.at[o - 1, e], xd_recv.at[o - 1, e],
            device_id=(gr, fs, tp_at(o)), device_id_type=MESH,
        )

    def down_own(e):
        return pltpu.make_async_copy(
            stage_down.at[0, e], down_out.at[e, :, down_block(gr, tp)], own_down_sem.at[e]
        )

    def down_over_gr(e, s, o, group):
        piece = down_out.at[e, :, down_block(group, lax.rem(tp - s + n_tp, n_tp))]
        return pltpu.make_async_remote_copy(
            piece, piece, dd_send.at[e, s, o - 1], dd_recv.at[e, s, o - 1],
            device_id=(lax.rem(gr + o, n_gr), fs, tp), device_id_type=MESH,
        )

    for w, o in order:
        load(0, w, o).start()
    for o in range(n_tp):
        load_down(0, o).start()
    pl.semaphore_wait(barrier, peers)

    @pl.loop(0, experts)
    def _(e):
        for w, o in order:
            load(e, w, o).wait()
            stage[w, o, e] = (raw[w, o] * gain_ref[...]).astype(BF16)

            @pl.when(e + 1 < experts)
            def _():
                load(e + 1, w, o).start()

            if o:
                over_tp(e, w, o).start()
            else:
                fan(e, w, 0)

    @pl.loop(0, experts)
    def _(e):
        for o in [*range(1, n_tp), 0]:
            load_down(e, o).wait()
            stage_down[o, e] = raw_down[o].astype(BF16)

            @pl.when(e + 1 < experts)
            def _():
                load_down(e + 1, o).start()

            if o:
                down_over_tp(e, o).start()
            else:
                down_own(e).start()

    def forward(e):
        for w in range(2):
            for o in range(1, n_tp):
                over_tp(e, w, o).wait_recv()
                fan(e, w, o)

    def collect(e):
        for w in range(2):
            own_copy(e, w).wait()
            for o in range(1, n_gr):
                over_gr(e, w, 0, o, gr).start()

        @pl.loop(1, n_fs)
        def _(k):
            for w in range(2):
                arrival(e, w, k).wait_recv()
                for o in range(1, n_gr):
                    over_gr(e, w, k, o, gr).start()

    forward(0)

    @pl.loop(1, experts)
    def _(e):
        forward(e)
        collect(e - 1)

    @pl.loop(0, experts)
    def _(e):
        down_own(e).wait()
        for s in range(1, n_tp):
            down_arrival(e, s).wait_recv()
        for s in range(n_tp):
            for o in range(1, n_gr):
                down_over_gr(e, s, o, gr).start()

    collect(experts - 1)

    @pl.loop(0, experts)
    def _(e):
        for w in range(2):
            for o in range(1, n_tp):
                over_tp(e, w, o).wait_send()

            @pl.loop(1, n_fs)
            def _(k):
                arrival(e, w, k).wait_send()

            @pl.loop(0, n_fs)
            def _(k):
                for o in range(1, n_gr):
                    over_gr(e, w, k, o, gr).wait_send()
                    over_gr(e, w, k, o, lax.rem(gr - o + n_gr, n_gr)).wait_recv()

        for s in range(1, n_tp):
            down_over_tp(e, s).wait_send()
        for s in range(n_tp):
            for o in range(1, n_gr):
                down_over_gr(e, s, o, gr).wait_send()
                down_over_gr(e, s, o, lax.rem(gr - o + n_gr, n_gr)).wait_recv()


def exchange(sizes, norm_gain, gate_master, up_master, down_master):
    n_gr, n_fs, n_tp = sizes
    all_experts, rows, cols = gate_master.shape
    experts = all_experts // n_tp
    width = cols * n_tp // n_fs
    hidden, down_cols = down_master.shape[1], down_master.shape[2]
    any_spec = pl.BlockSpec(memory_space=pl.ANY)
    dma = pltpu.SemaphoreType.DMA
    up_shape = jax.ShapeDtypeStruct((experts, rows * n_gr * n_fs, width), BF16)
    return pl.pallas_call(
        functools.partial(exchange_kernel, n_gr, n_fs, n_tp),
        out_shape=(
            up_shape,
            up_shape,
            jax.ShapeDtypeStruct((experts, hidden, down_cols * n_gr * n_tp), BF16),
        ),
        in_specs=[pl.BlockSpec(memory_space=pltpu.VMEM), any_spec, any_spec, any_spec],
        out_specs=(any_spec, any_spec, any_spec),
        scratch_shapes=[
            pltpu.VMEM((2, n_tp, experts, rows, cols), BF16),
            pltpu.VMEM((n_tp, experts, hidden, down_cols), BF16),
            pltpu.VMEM((2, n_tp - 1, experts, rows, cols), BF16),
            pltpu.VMEM((2, n_tp, rows, cols), jnp.float32),
            pltpu.VMEM((n_tp, hidden, down_cols), jnp.float32),
            dma((2, n_tp)),
            dma((n_tp,)),
            dma((2, n_tp - 1, experts)),
            dma((2, n_tp - 1, experts)),
            dma((2, experts, n_fs)),
            dma((2, experts, n_fs)),
            dma((2, experts)),
            dma((2, experts, n_fs, n_gr - 1)),
            dma((2, experts, n_fs, n_gr - 1)),
            dma((n_tp - 1, experts)),
            dma((n_tp - 1, experts)),
            dma((experts,)),
            dma((experts, n_tp, n_gr - 1)),
            dma((experts, n_tp, n_gr - 1)),
        ],
        compiler_params=pltpu.CompilerParams(
            collective_id=0, has_side_effects=True, vmem_limit_bytes=52 * 1024 * 1024
        ),
        cost_estimate=pl.CostEstimate(flops=0, bytes_accessed=1_000_000_000, transcendentals=0),
    )(norm_gain[:, None], gate_master, up_master, down_master)


def experts_kernel(pieces, gate_in, up_in, down_in, gate_out, up_out, down_out, partial, gate_act, up_act, hidden):
    depth = 256
    gate_act[...] = jnp.zeros_like(gate_act)
    up_act[...] = jnp.zeros_like(up_act)

    @pl.loop(0, gate_in.shape[1] // depth)
    def _(i):
        span = pl.ds(pl.multiple_of(i * depth, depth), depth)
        x = pieces[0, :, span]
        gate = gate_in[0, span, :]
        gate_out[0, span, :] = gate
        gate_act[...] += jnp.dot(x, gate, preferred_element_type=jnp.float32)
        up = up_in[0, span, :]
        up_out[0, span, :] = up
        up_act[...] += jnp.dot(x, up, preferred_element_type=jnp.float32)

    hidden[...] = (jax.nn.silu(gate_act[...]) * up_act[...]).astype(BF16)

    @pl.loop(0, down_in.shape[2] // depth)
    def _(i):
        span = pl.ds(pl.multiple_of(i * depth, depth), depth)
        down = down_in[0, :, span]
        down_out[0, :, span] = down
        partial[0, :, span] = jnp.dot(
            hidden[...], down, preferred_element_type=jnp.float32
        ).astype(BF16)


def run_experts(pieces, gate, up, down):
    experts, features, width = gate.shape
    count = pieces.shape[1]

    def whole(*shape):
        return pl.BlockSpec((1, *shape), lambda e: (e, 0, 0))

    weights = [whole(features, width), whole(features, width), whole(width, features)]
    return pl.pallas_call(
        experts_kernel,
        grid=(experts,),
        out_shape=(
            jax.ShapeDtypeStruct(gate.shape, BF16),
            jax.ShapeDtypeStruct(up.shape, BF16),
            jax.ShapeDtypeStruct(down.shape, BF16),
            jax.ShapeDtypeStruct(pieces.shape, BF16),
        ),
        in_specs=[whole(count, features), *weights],
        out_specs=(*weights, whole(count, features)),
        scratch_shapes=[
            pltpu.VMEM((count, width), jnp.float32),
            pltpu.VMEM((count, width), jnp.float32),
            pltpu.VMEM((count, width), BF16),
        ],
        compiler_params=pltpu.CompilerParams(vmem_limit_bytes=60 * 1024 * 1024),
    )(pieces, gate, up, down)


def combine_kernel(
    n_fs, n_tp, part, combiner, out,
    near, summed, far, total, block, others,
    y_send, y_recv, z_send, z_recv, t_send, t_recv,
):
    gr, fs, tp = (lax.axis_index(name) for name in ("gr", "fs", "tp"))
    pairs = n_fs // 2
    z, y = fs // 2, lax.rem(fs, 2)
    experts, _, _, cap, features = part.shape

    barrier = pltpu.get_barrier_semaphore()
    pl.semaphore_signal(barrier, 1, device_id=(gr, z * 2 + 1 - y, tp), device_id_type=MESH)
    for k in range(1, pairs):
        pl.semaphore_signal(
            barrier, 1, device_id=(gr, lax.rem(z + k, pairs) * 2 + y, tp), device_id_type=MESH
        )
    for o in range(1, n_tp):
        pl.semaphore_signal(barrier, 1, device_id=(gr, fs, lax.rem(tp + o, n_tp)), device_id_type=MESH)
    pl.semaphore_wait(barrier, pairs + n_tp - 1)

    def over_pair(e):
        return pltpu.make_async_remote_copy(
            part.at[e, :, 1 - y], near.at[e], y_send.at[e], y_recv.at[e],
            device_id=(gr, z * 2 + 1 - y, tp), device_id_type=MESH,
        )

    def over_pairs(e, k):
        to = lax.rem(z + k, pairs)
        return pltpu.make_async_remote_copy(
            summed.at[e, to], far.at[k - 1, e], z_send.at[k - 1, e], z_recv.at[k - 1, e],
            device_id=(gr, to * 2 + y, tp), device_id_type=MESH,
        )

    def over_tp(o):
        return pltpu.make_async_remote_copy(
            block, others.at[o - 1], t_send.at[o - 1], t_recv.at[o - 1],
            device_id=(gr, fs, lax.rem(tp + o, n_tp)), device_id_type=MESH,
        )

    @pl.loop(0, experts)
    def _(e):
        over_pair(e).start()

    @pl.loop(0, experts)
    def _(e):
        over_pair(e).wait_recv()
        summed[e] = (part[e, :, y].astype(jnp.float32) + near[e].astype(jnp.float32)).astype(BF16)
        for k in range(1, pairs):
            over_pairs(e, k).start()

    @pl.loop(0, experts)
    def _(e):
        value = summed[e, z].astype(jnp.float32)
        for k in range(1, pairs):
            over_pairs(e, k).wait_recv()
            value = value + far[k - 1, e].astype(jnp.float32)
        total[pl.ds(pl.multiple_of(e * cap, cap), cap), :] = value

    tile = 512

    @pl.loop(0, features // tile)
    def _(i):
        span = pl.ds(pl.multiple_of(i * tile, tile), tile)
        block[:, span] = jnp.dot(
            combiner[...], total[:, span], preferred_element_type=jnp.float32,
            precision=lax.Precision.HIGHEST,
        ).astype(BF16)

    for o in range(1, n_tp):
        over_tp(o).start()
    mixed = block[...].astype(jnp.float32)
    for o in range(1, n_tp):
        over_tp(o).wait_recv()
        mixed = mixed + others[o - 1].astype(jnp.float32)
    out[...] = mixed.astype(BF16)

    @pl.loop(0, experts)
    def _(e):
        over_pair(e).wait_send()
        for k in range(1, pairs):
            over_pairs(e, k).wait_send()

    for o in range(1, n_tp):
        over_tp(o).wait_send()


def combine(n_fs, n_tp, partial, combiner):
    experts, count, features = partial.shape
    pairs, cap, tokens = n_fs // 2, count // n_fs, combiner.shape[0]
    dma = pltpu.SemaphoreType.DMA
    vmem = pl.BlockSpec(memory_space=pltpu.VMEM)
    return pl.pallas_call(
        functools.partial(combine_kernel, n_fs, n_tp),
        out_shape=jax.ShapeDtypeStruct((tokens, features), BF16),
        in_specs=[vmem, vmem],
        out_specs=vmem,
        scratch_shapes=[
            pltpu.VMEM((experts, pairs, cap, features), BF16),
            pltpu.VMEM((experts, pairs, cap, features), BF16),
            pltpu.VMEM((pairs - 1, experts, cap, features), BF16),
            pltpu.VMEM((experts * cap, features), jnp.float32),
            pltpu.VMEM((tokens, features), BF16),
            pltpu.VMEM((n_tp - 1, tokens, features), BF16),
            dma((experts,)),
            dma((experts,)),
            dma((pairs - 1, experts)),
            dma((pairs - 1, experts)),
            dma((n_tp - 1,)),
            dma((n_tp - 1,)),
        ],
        compiler_params=pltpu.CompilerParams(
            collective_id=1, has_side_effects=True, vmem_limit_bytes=40 * 1024 * 1024
        ),
    )(partial.reshape(experts, pairs, 2, cap, features), combiner)


def plain_local(tokens, route_ids, route_logits, norm_gain, gate_master, up_master, down_master):
    gain_rows = norm_gain[None, :, None]
    gate_half = (gate_master * gain_rows).astype(jnp.bfloat16)
    up_half = (up_master * gain_rows).astype(jnp.bfloat16)
    down_half = down_master.astype(jnp.bfloat16)
    gate_cols, up_cols, down_cols = (
        lax.all_to_all(gate_half, "tp", split_axis=0, concat_axis=2, tiled=True),
        lax.all_to_all(up_half, "tp", split_axis=0, concat_axis=2, tiled=True),
        lax.all_to_all(down_half, "tp", split_axis=0, concat_axis=2, tiled=True),
    )
    gate_part, up_part = (
        lax.all_to_all(gate_cols, "fs", split_axis=2, concat_axis=1, tiled=True),
        lax.all_to_all(up_cols, "fs", split_axis=2, concat_axis=1, tiled=True),
    )
    gate_weight, up_weight, down_weight = (
        lax.all_gather(gate_part, "gr", axis=1, tiled=True),
        lax.all_gather(up_part, "gr", axis=1, tiled=True),
        lax.all_gather(down_cols, "gr", axis=2, tiled=True),
    )
    as_float = tokens.astype(jnp.float32)
    normed = (
        as_float * lax.rsqrt(jnp.mean(as_float * as_float, axis=-1, keepdims=True) + epsilon)
    ).astype(jnp.bfloat16)
    differ = route_logits[:, 0] - route_logits[:, 1]
    route_weight = jnp.stack([jax.nn.sigmoid(differ), jax.nn.sigmoid(-differ)], axis=1)
    experts_here = gate_weight.shape[0]
    first_expert = lax.axis_index("tp") * experts_here
    expert_ids = first_expert + jnp.arange(experts_here, dtype=jnp.int32)
    route_hits = route_ids[None, :, :] == expert_ids[:, None, None]
    chosen = jnp.any(route_hits, axis=2)
    weight_rows = jnp.sum(jnp.where(route_hits, route_weight[None, :, :], 0.0), axis=2)
    slot_rank = jnp.cumsum(chosen.astype(jnp.int32), axis=1) - 1
    slot_ids = jnp.arange(CAP, dtype=jnp.int32)
    picker = chosen[:, None, :] & (slot_rank[:, None, :] == slot_ids[None, :, None])
    picker_float = picker.astype(jnp.float32)
    packed = jnp.einsum(
        "xsr,rd->sxd", picker.astype(jnp.bfloat16), normed, preferred_element_type=jnp.float32
    ).astype(jnp.bfloat16)
    slot_weight = jnp.einsum(
        "xsr,xr->sx", picker_float, weight_rows, precision=lax.Precision.HIGHEST
    )
    pieces = lax.all_gather(packed, "fs", axis=0, tiled=True)
    gate_act = jnp.einsum("kxd,xdh->kxh", pieces, gate_weight, preferred_element_type=jnp.float32)
    up_act = jnp.einsum("kxd,xdh->kxh", pieces, up_weight, preferred_element_type=jnp.float32)
    hidden = (jax.nn.silu(gate_act) * up_act).astype(jnp.bfloat16)
    expert_out = lax.psum_scatter(
        jnp.einsum("kxh,xhd->kxd", hidden, down_weight, preferred_element_type=jnp.float32).astype(
            jnp.bfloat16
        ),
        "fs",
        scatter_dimension=0,
        tiled=True,
    ).astype(jnp.float32)
    weighted = expert_out * slot_weight[:, :, None]
    block_sum = jnp.einsum("xsr,sxd->rd", picker_float, weighted, precision=lax.Precision.HIGHEST)
    mixed = lax.psum(block_sum.astype(jnp.bfloat16), "tp")
    return (gate_weight, up_weight, down_weight, mixed)


def fast_local(sizes, tokens, route_ids, route_logits, norm_gain, gate_master, up_master, down_master):
    n_gr, n_fs, n_tp = sizes
    gate_moved, up_moved, down_moved = exchange(
        sizes, norm_gain, gate_master, up_master, down_master
    )
    as_float = tokens.astype(jnp.float32)
    normed = (
        as_float * lax.rsqrt(jnp.mean(as_float * as_float, axis=-1, keepdims=True) + epsilon)
    ).astype(jnp.bfloat16)
    differ = route_logits[:, 0] - route_logits[:, 1]
    route_weight = jnp.stack([jax.nn.sigmoid(differ), jax.nn.sigmoid(-differ)], axis=1)
    experts_here = gate_moved.shape[0]
    first_expert = lax.axis_index("tp") * experts_here
    expert_ids = first_expert + jnp.arange(experts_here, dtype=jnp.int32)
    route_hits = route_ids[None, :, :] == expert_ids[:, None, None]
    chosen = jnp.any(route_hits, axis=2)
    weight_rows = jnp.sum(jnp.where(route_hits, route_weight[None, :, :], 0.0), axis=2)
    slot_rank = jnp.cumsum(chosen.astype(jnp.int32), axis=1) - 1
    slot_ids = jnp.arange(CAP, dtype=jnp.int32)
    picker = chosen[:, None, :] & (slot_rank[:, None, :] == slot_ids[None, :, None])
    picker_float = picker.astype(jnp.float32)
    packed = jnp.einsum(
        "xsr,rd->xsd", picker.astype(jnp.bfloat16), normed, preferred_element_type=jnp.float32
    ).astype(jnp.bfloat16)
    combiner = jnp.transpose(picker_float * weight_rows[:, None, :], (2, 0, 1))
    pieces = lax.all_gather(packed, "fs", axis=1, tiled=True)
    gate_weight, up_weight, down_weight, partial = run_experts(
        pieces, gate_moved, up_moved, down_moved
    )
    mixed = combine(n_fs, n_tp, partial, combiner.reshape(combiner.shape[0], -1))
    return (gate_weight, up_weight, down_weight, mixed)


def solution(mesh):
    n_gr, n_fs, n_tp = (mesh.shape[name] for name in ("gr", "fs", "tp"))
    placed = (
        P(("gr", "fs"), None),
        P(("gr", "fs"), None),
        P(("gr", "fs"), None),
        P(("gr", "fs")),
        P(None, ("gr", "fs"), "tp"),
        P(None, ("gr", "fs"), "tp"),
        P(None, "fs", ("gr", "tp")),
    )

    def local(tokens, route_ids, route_logits, norm_gain, gate_master, up_master, down_master):
        width = gate_master.shape[2] * n_tp // n_fs
        aligned = width % 128 == 0 and down_master.shape[2] % 128 == 0
        fits = n_fs % n_tp == 0 and n_fs % 2 == 0 and min(n_gr, n_tp) > 1
        run = functools.partial(fast_local, (n_gr, n_fs, n_tp)) if aligned and fits else plain_local
        return run(tokens, route_ids, route_logits, norm_gain, gate_master, up_master, down_master)

    return jax.shard_map(
        local,
        mesh=mesh,
        in_specs=placed,
        out_specs=(
            P("tp", None, "fs"),
            P("tp", None, "fs"),
            P("tp", "fs", None),
            P(("gr", "fs"), None),
        ),
        check_vma=False,
    )
```
